32 devices in a mesh: sp: 8 (over z, y), tp: 4 (over x, core).
Axes of the slice: x: 2, y: 2, z: 4, core: 2. Of those that a mesh axis runs over, the one named last changes fastest.
Arguments:
- queries: bfloat16 [6144, 1024], P('sp', 'tp'), may hold values from -8 to 8
- keys: bfloat16 [6144, 256], P('sp', 'tp'), may hold values from -8 to 8
- values: bfloat16 [6144, 256], P('sp', 'tp'), may hold values from -18 to 18
- query_gain: float32 [64], replicated, may hold values from 0.4 to 5.5
- key_gain: float32 [64], replicated, may hold values from 0.4 to 5.5
- sink_logits: float32 [16], P('tp'), may hold values from 2 to 5
- out_weight: bfloat16 [1024, 2048], P('tp'), may hold values from -0.1875 to 0.1875
- residual: bfloat16 [6144, 2048], P('sp', 'tp'), may hold values from -21 to 21
- norm_gain: float32 [2048], P('tp'), may hold values from 0.1 to 1.9
- gate_weight: bfloat16 [2048, 5632], P('sp', 'tp'), may hold values from -0.125 to 0.125
- up_weight: bfloat16 [2048, 5632], P('sp', 'tp'), may hold values from -0.125 to 0.125
- down_weight: bfloat16 [5632, 2048], P('tp', 'sp'), may hold values from -0.078125 to 0.078125
Outputs:
- layer_out: bfloat16 [6144, 2048], P('sp', 'tp')
The draws below stay inside these ranges and needn't reach their ends.
All inputs are finite; a program needn't handle non-finite values.
Results may differ from the reference program's by a relative error of at most 0.0095.
The reference program's roundings to bfloat16 on the way count: a program that leaves them out, or rounds other values in their place, can miss the bound.
Values may be sent and summed in bfloat16 or wider, within the bound.
A program may use at most 192 MiB of HBM per device.

```python
import jax
import jax.numpy as jnp
from jax import lax

D = 2048
FF = 5632
HEAD_DIM = 64
Q_HEADS = 16
KV_HEADS = 4
WINDOW = 128
TOKENS = 6144
N_TP = 4


def shared_fields(key):
    key_rows = jnp.clip(jax.random.normal(jax.random.fold_in(key, 101), (TOKENS, KV_HEADS * HEAD_DIM), jnp.float32), -6.0, 6.0)
    query_rows = jnp.clip(jax.random.normal(jax.random.fold_in(key, 102), (TOKENS, Q_HEADS * HEAD_DIM), jnp.float32), -6.0, 6.0)
    return (key_rows, query_rows)


def draw_keys(key, part):
    return shared_fields(key)[0].astype(jnp.bfloat16)


def draw_queries(key, part):
    return shared_fields(key)[1].astype(jnp.bfloat16)


def gain_draw(key):
    return 1.0 + 0.18 * jnp.clip(jax.random.normal(key, (HEAD_DIM,), jnp.float32), -3.0, 3.0)


def draw_query_gain(key, part):
    return gain_draw(jax.random.fold_in(key, 104))


def draw_key_gain(key, part):
    return gain_draw(jax.random.fold_in(key, 105))


def draw_residual(key, part):
    columns = jnp.arange(D).astype(jnp.float32)
    col_scale = 3.0 ** (columns / (D - 1))
    base = jnp.clip(jax.random.normal(jax.random.fold_in(key, 106), (TOKENS, D), jnp.float32), -6.0, 6.0)
    return (base * col_scale).astype(jnp.bfloat16)


def shard_levels(own_key, shape, pieces, low, top_value):
    factor_of, own = 1.0, jax.random.fold_in(own_key, 6)
    for dim, blocks in pieces:
        steps = jnp.exp(jax.random.uniform(jax.random.fold_in(own, dim), (blocks,), jnp.float32, low / len(pieces), top_value / len(pieces)))
        factor_of = factor_of * jnp.repeat(steps, shape[dim] // blocks).reshape([-1 if axis == dim else 1 for axis in range(len(shape))])
    return factor_of


def bell_draw(own_key, extent, scale, reach, pieces=(), kind=jnp.bfloat16):
    result = jax.random.normal(own_key, extent, jnp.float32) * scale
    if len(pieces) > 0:
        result = shard_levels(own_key, extent, pieces, -0.22, 0.18) * result
    return jnp.clip(result, min=-reach, max=reach).astype(kind)


def setup_inputs(seed: int = 0) -> dict:
    splits = jax.random.split(jax.random.key(seed), 13)
    return {
        "queries": draw_queries(jax.random.fold_in(splits[12], 71), 0),
        "keys": draw_keys(jax.random.fold_in(splits[12], 71), 0),
        "values": bell_draw(splits[2], (TOKENS, KV_HEADS * HEAD_DIM), 3.0, 18.0, ((0, 8), (1, 4))),
        "query_gain": draw_query_gain(jax.random.fold_in(splits[12], 71), 0),
        "key_gain": draw_key_gain(jax.random.fold_in(splits[12], 71), 0),
        "sink_logits": jnp.clip(2.0 + 3.0 * jax.random.uniform(splits[5], (Q_HEADS,), jnp.float32) ** shard_levels(splits[5], (Q_HEADS,), ((0, 4),), -0.2, 0.2), 2.0, 5.0),
        "out_weight": bell_draw(splits[6], (Q_HEADS * HEAD_DIM, D), (Q_HEADS * HEAD_DIM) ** -0.5, 0.1875, ((0, 4),)),
        "residual": draw_residual(jax.random.fold_in(splits[12], 71), 0),
        "norm_gain": jnp.clip(1.0 + 0.18 * jax.random.normal(splits[8], (D,), jnp.float32), 0.1, 1.9),
        "gate_weight": bell_draw(splits[9], (D, FF), D ** -0.5, 0.125, ((0, 8), (1, 4))),
        "up_weight": bell_draw(splits[10], (D, FF), D ** -0.5, 0.125, ((0, 8), (1, 4))),
        "down_weight": bell_draw(splits[11], (FF, D), FF ** -0.5, 0.078125, ((0, 4), (1, 8))),
    }


def norm_heads(flat, gain, heads):
    row_count = flat.shape[0]
    head_width = gain.shape[0]
    data = flat.astype(jnp.float32).reshape(row_count, heads, head_width)
    scaled = data * lax.rsqrt(lax.optimization_barrier(jnp.mean(data * data, axis=-1, keepdims=True)) + 1e-06) * gain
    return scaled.astype(jnp.bfloat16)

def reference(queries, keys, values, query_gain, key_gain, sink_logits, out_weight, residual, norm_gain, gate_weight, up_weight, down_weight):
    seq_len = queries.shape[0]
    group_size = Q_HEADS // KV_HEADS
    block_count = seq_len // WINDOW
    query_heads = norm_heads(queries, query_gain, Q_HEADS).reshape(seq_len, KV_HEADS, group_size, HEAD_DIM).transpose(1, 0, 2, 3)
    key_heads = norm_heads(keys, key_gain, KV_HEADS).transpose(1, 0, 2)
    value_heads = values.reshape(seq_len, KV_HEADS, HEAD_DIM).transpose(1, 0, 2)
    sink_rows = sink_logits.reshape(KV_HEADS, group_size)
    query_index = jnp.arange(WINDOW)[:, None]
    key_index = jnp.arange(2 * WINDOW)[None, :]
    offset_lag = WINDOW + query_index - key_index
    inband = (offset_lag >= 0) & (offset_lag < WINDOW)
    leading = (jnp.arange(block_count)[:, None, None] > 0) | (key_index[None] >= WINDOW)
    valid = inband[None] & leading

    def one_head(operands):
        query_h, key_h, value_h, sink_h = operands
        zero_rows = jnp.zeros((WINDOW, HEAD_DIM), jnp.bfloat16)
        key_prev = jnp.concatenate([zero_rows, key_h[:seq_len - WINDOW]], axis=0)
        value_prev = jnp.concatenate([zero_rows, value_h[:seq_len - WINDOW]], axis=0)
        key_blocks = jnp.concatenate([key_prev.reshape(block_count, WINDOW, HEAD_DIM), key_h.reshape(block_count, WINDOW, HEAD_DIM)], axis=1).astype(jnp.float32)
        value_blocks = jnp.concatenate([value_prev.reshape(block_count, WINDOW, HEAD_DIM), value_h.reshape(block_count, WINDOW, HEAD_DIM)], axis=1).astype(jnp.float32)
        query_blocks = query_h.reshape(block_count, WINDOW, group_size, HEAD_DIM).astype(jnp.float32)
        scores = jnp.einsum('nqgd,nkd->ngqk', query_blocks, key_blocks) * HEAD_DIM ** (-0.5)
        scores = jnp.where(valid[:, None], scores, -1e+30)
        sink_b = sink_h[None, :, None]
        row_peak = jnp.maximum(lax.optimization_barrier(jnp.max(scores, axis=-1)), sink_b)
        exp_terms = jnp.exp(scores - row_peak[..., None])
        denom_sum = lax.optimization_barrier(jnp.sum(exp_terms, axis=-1)) + jnp.exp(sink_b - row_peak)
        weights = (exp_terms / denom_sum[..., None]).astype(jnp.bfloat16)
        attended = jnp.einsum('ngqk,nkd->nqgd', weights.astype(jnp.float32), value_blocks).astype(jnp.bfloat16)
        return attended.reshape(seq_len, group_size, HEAD_DIM)
    heads_out = lax.map(one_head, (query_heads, key_heads, value_heads, sink_rows))
    attended = heads_out.transpose(1, 0, 2, 3).reshape(seq_len, Q_HEADS * HEAD_DIM)
    slice_width = Q_HEADS * HEAD_DIM // N_TP
    mixed = jnp.zeros((seq_len, D), jnp.float32)
    for member in range(N_TP):
        lower = member * slice_width
        product = jnp.dot(attended[:, lower:lower + slice_width], out_weight[lower:lower + slice_width], preferred_element_type=jnp.float32)
        mixed = mixed + product.astype(jnp.bfloat16).astype(jnp.float32)
    middle = (residual.astype(jnp.float32) + mixed).astype(jnp.bfloat16)
    middle_wide = middle.astype(jnp.float32)
    normed = (middle_wide * lax.rsqrt(lax.optimization_barrier(jnp.mean(middle_wide * middle_wide, axis=1, keepdims=True)) + 1e-06) * norm_gain).astype(jnp.bfloat16)
    hidden_width = FF // N_TP
    feed = jnp.zeros((seq_len, D), jnp.float32)
    for member in range(N_TP):
        lower = member * hidden_width
        gate_acts = jnp.dot(normed, gate_weight[:, lower:lower + hidden_width], preferred_element_type=jnp.float32)
        up_acts = jnp.dot(normed, up_weight[:, lower:lower + hidden_width], preferred_element_type=jnp.float32)
        hidden = (jax.nn.silu(gate_acts) * up_acts).astype(jnp.bfloat16)
        product = jnp.dot(hidden, down_weight[lower:lower + hidden_width], preferred_element_type=jnp.float32)
        feed = feed + product.astype(jnp.bfloat16).astype(jnp.float32)
    return (middle_wide + 0.5 * feed).astype(jnp.bfloat16)
```

```python
import jax
import jax.numpy as jnp
from jax import lax
from jax.sharding import PartitionSpec as P

WINDOW = 128
PAIR = 2


def swap(block, axis, flip):
    return lax.ppermute(block, axis, [(i, i ^ flip) for i in range(lax.axis_size(axis))])


def from_behind(block, axis, distance):
    devices = range(lax.axis_size(axis))
    route = [(i - distance, i) for i in devices if i - distance in devices]
    return lax.ppermute(block, axis, route)


def gather_flips(block, axis):
    found = {0: block}
    flip = lax.axis_size(axis) // 2
    while flip:
        for at, held in list(found.items()):
            found[at ^ flip] = swap(held, axis, flip)
        flip //= 2
    return [found[at] for at in range(lax.axis_size(axis))]


def norm_heads(flat, gain, heads):
    row_count = flat.shape[0]
    head_width = gain.shape[0]
    data = flat.astype(jnp.float32).reshape(row_count, heads, head_width)
    scaled = data * lax.rsqrt(jnp.mean(data * data, axis=-1, keepdims=True) + 1e-06) * gain
    return scaled.astype(jnp.bfloat16)


def attend(queries, keys, values, query_gain, key_gain, sink_logits):
    head_width = query_gain.shape[0]
    row_count = queries.shape[0]
    q_heads = queries.shape[1] // head_width
    k_heads = keys.shape[1] // head_width
    group_size = q_heads // k_heads
    window_len = WINDOW
    block_count = row_count // window_len
    edge = jnp.concatenate([keys, values], axis=1)[row_count - window_len :]
    edge = from_behind(edge, "sp", 1)
    query_norm = norm_heads(queries, query_gain, q_heads)
    key_raw = jnp.concatenate([edge[:, : keys.shape[1]], keys], axis=0)
    key_all = norm_heads(key_raw, key_gain, k_heads).reshape(key_raw.shape)
    value_all = jnp.concatenate([edge[:, keys.shape[1] :], values], axis=0)

    def windows(flat):
        return jnp.concatenate(
            [
                flat[:row_count].reshape(block_count, window_len, k_heads, head_width),
                flat[window_len:].reshape(block_count, window_len, k_heads, head_width),
            ],
            axis=1,
        )

    key_blocks, value_blocks = windows(key_all), windows(value_all)
    query_blocks = query_norm.reshape(block_count, window_len, k_heads, group_size, head_width)
    scores = jnp.einsum(
        "nqhgd,nkhd->nhgqk", query_blocks, key_blocks, preferred_element_type=jnp.float32
    ) * head_width ** (-0.5)
    query_index = jnp.arange(window_len)[:, None]
    key_index = jnp.arange(2 * window_len)[None, :]
    offset_lag = window_len + query_index - key_index
    inband = (offset_lag >= 0) & (offset_lag < window_len)
    leading = (
        (jnp.arange(block_count)[:, None, None] > 0)
        | (key_index[None] >= window_len)
        | (lax.axis_index("sp") > 0)
    )
    valid = inband[None] & leading
    scores = jnp.where(valid[:, None, None], scores, -1e30)
    sink_rows = sink_logits.reshape(k_heads, group_size)[None, :, :, None]
    row_peak = jnp.maximum(jnp.max(scores, axis=-1), sink_rows)
    exp_terms = jnp.exp(scores - row_peak[..., None])
    denom_sum = jnp.sum(exp_terms, axis=-1) + jnp.exp(sink_rows - row_peak)
    weights = (exp_terms / denom_sum[..., None]).astype(jnp.bfloat16)
    attended = jnp.einsum(
        "nhgqk,nkhd->nqhgd", weights, value_blocks, preferred_element_type=jnp.float32
    ).astype(jnp.bfloat16)
    return attended.reshape(row_count, q_heads * head_width)


def per_device(
    queries,
    keys,
    values,
    query_gain,
    key_gain,
    sink_logits,
    out_weight,
    residual,
    norm_gain,
    gate_weight,
    up_weight,
    down_weight,
):
    n_sp, n_tp = lax.axis_size("sp"), lax.axis_size("tp")
    sp, tp = lax.axis_index("sp"), lax.axis_index("tp")
    half = (sp // PAIR) % 2
    row_count, width = residual.shape
    depth, units = gate_weight.shape
    units //= 2

    def part(array, axis, flip):
        return lax.dynamic_slice_in_dim(array, (half ^ flip) * units, units, axis)

    far = list(range(2 * PAIR, n_sp, 2))

    def send_rows(array, axis, flips):
        found = {}
        for flip in flips:
            piece = part(array, axis, (flip // PAIR) % 2)
            found[flip] = swap(piece, "sp", flip) if flip else piece
        return found

    residual_pair = swap(residual, "sp", PAIR)
    gate = send_rows(gate_weight, 1, far)
    attended = attend(queries, keys, values, query_gain, key_gain, sink_logits)
    attended_pair = swap(attended, "sp", PAIR)

    up_weight, gate = lax.optimization_barrier((up_weight, gate))
    up = send_rows(up_weight, 1, far)
    down_weight, up = lax.optimization_barrier((down_weight, up))
    down = send_rows(down_weight, 0, far)

    near = [0, PAIR]
    gate.update(send_rows(gate_weight, 1, near))
    up.update(send_rows(up_weight, 1, near))
    down.update(send_rows(down_weight, 0, near))
    for found in (gate, up, down):
        for flip in near + far:
            found[flip ^ 1] = swap(found[flip], "sp", 1)

    gains = jnp.concatenate(gather_flips(norm_gain, "tp"))
    projections = gather_flips(out_weight, "tp")
    streams = [
        jnp.concatenate(gather_flips(rows, "tp"), axis=1) for rows in (residual, residual_pair)
    ]
    stream = jnp.concatenate(streams, axis=0).astype(jnp.float32)
    heads = [
        jnp.concatenate(pieces, axis=0)
        for pieces in zip(gather_flips(attended, "tp"), gather_flips(attended_pair, "tp"))
    ]

    def own_first(columns):
        pieces = [
            lax.dynamic_slice_in_dim(columns, (tp ^ flip) * width, width, 1)
            for flip in range(n_tp)
        ]
        return jnp.concatenate(pieces, axis=1)

    mixed = 0.0
    for head, projection in zip(heads, projections):
        product = jnp.dot(head, own_first(projection), preferred_element_type=jnp.float32)
        mixed = mixed + product.astype(jnp.bfloat16).astype(jnp.float32)
    middle = (stream + mixed).astype(jnp.bfloat16)
    middle_wide = middle.astype(jnp.float32)
    mean = jnp.mean(middle_wide * middle_wide, axis=1, keepdims=True)
    normed = (middle_wide * lax.rsqrt(mean + 1e-06) * gains).astype(jnp.bfloat16)

    per_part = width // depth

    def place(flip):
        block = sp ^ flip
        return (((block // per_part) ^ tp) * per_part + block % per_part) * depth

    flips = range(n_sp)
    normed_in = jnp.concatenate(
        [lax.dynamic_slice_in_dim(normed, place(flip), depth, 1) for flip in flips], axis=1
    )
    gate_full = jnp.concatenate([gate[flip] for flip in flips], axis=0)
    up_full = jnp.concatenate([up[flip] for flip in flips], axis=0)
    gate_acts = jnp.dot(normed_in, gate_full, preferred_element_type=jnp.float32)
    up_acts = jnp.dot(normed_in, up_full, preferred_element_type=jnp.float32)
    hidden = (jax.nn.silu(gate_acts) * up_acts).astype(jnp.bfloat16)

    down_full = jnp.zeros((units, width * n_tp), jnp.bfloat16)
    for flip in flips:
        down_full = lax.dynamic_update_slice_in_dim(down_full, down[flip], place(flip), 1)
    terms = [
        jnp.dot(
            hidden, down_full[:, at * width : (at + 1) * width], preferred_element_type=jnp.float32
        ).astype(jnp.bfloat16)
        for at in range(n_tp)
    ]

    def add(one, other):
        return one.astype(jnp.float32) + other.astype(jnp.float32)

    flip = 1
    held = dict(enumerate(terms))
    while flip < n_tp // 2:
        held = {
            at: add(held[at], swap(held[at ^ flip], "tp", flip)).astype(jnp.bfloat16)
            for at in held
            if not at & flip
        }
        flip *= 2
    own, other = held[0], held[flip]
    cut = width // 2
    across = add(own[:, :cut], swap(other[:, :cut], "tp", flip)).astype(jnp.bfloat16)
    left = add(across[:row_count], swap(across[row_count:], "sp", PAIR))
    both = jnp.concatenate([own[:, cut:], other[:, cut:]], axis=1)
    both = add(both[:row_count], swap(both[row_count:], "sp", PAIR)).astype(jnp.bfloat16)
    right = add(both[:, : width - cut], swap(both[:, width - cut :], "tp", flip))
    feed = jnp.concatenate([left, right], axis=1)
    return (middle_wide[:row_count, :width] + 0.5 * feed).astype(jnp.bfloat16)


def solution(mesh):
    in_specs = (
        P("sp", "tp"),
        P("sp", "tp"),
        P("sp", "tp"),
        P(),
        P(),
        P("tp"),
        P("tp", None),
        P("sp", "tp"),
        P("tp"),
        P("sp", "tp"),
        P("sp", "tp"),
        P("tp", "sp"),
    )
    out_specs = P("sp", "tp")
    return jax.shard_map(
        per_device, mesh=mesh, in_specs=in_specs, out_specs=out_specs, check_vma=False
    )
```

```python
import jax
import jax.numpy as jnp
from jax import lax
from jax.sharding import PartitionSpec as P

WINDOW = 128
PAIR = 2


def swap(block, axis, flip):
    return lax.ppermute(block, axis, [(i, i ^ flip) for i in range(lax.axis_size(axis))])


def from_behind(block, axis, distance):
    devices = range(lax.axis_size(axis))
    route = [(i - distance, i) for i in devices if i - distance in devices]
    return lax.ppermute(block, axis, route)


def gather_flips(block, axis):
    found = {0: block}
    flip = lax.axis_size(axis) // 2
    while flip:
        for at, held in list(found.items()):
            found[at ^ flip] = swap(held, axis, flip)
        flip //= 2
    return [found[at] for at in range(lax.axis_size(axis))]


def norm_heads(flat, gain, heads):
    row_count = flat.shape[0]
    head_width = gain.shape[0]
    data = flat.astype(jnp.float32).reshape(row_count, heads, head_width)
    scaled = data * lax.rsqrt(jnp.mean(data * data, axis=-1, keepdims=True) + 1e-06) * gain
    return scaled.astype(jnp.bfloat16)


def attend(queries, keys, values, edge, query_gain, key_gain, sink_logits):
    head_width = query_gain.shape[0]
    row_count = queries.shape[0]
    q_heads = queries.shape[1] // head_width
    k_heads = keys.shape[1] // head_width
    group_size = q_heads // k_heads
    window_len = WINDOW
    block_count = row_count // window_len
    query_norm = norm_heads(queries, query_gain, q_heads)
    key_raw = jnp.concatenate([edge[:, : keys.shape[1]], keys], axis=0)
    key_all = norm_heads(key_raw, key_gain, k_heads).reshape(key_raw.shape)
    value_all = jnp.concatenate([edge[:, keys.shape[1] :], values], axis=0)

    def windows(flat):
        return jnp.concatenate(
            [
                flat[:row_count].reshape(block_count, window_len, k_heads, head_width),
                flat[window_len:].reshape(block_count, window_len, k_heads, head_width),
            ],
            axis=1,
        )

    key_blocks, value_blocks = windows(key_all), windows(value_all)
    query_blocks = query_norm.reshape(block_count, window_len, k_heads, group_size, head_width)
    scores = jnp.einsum(
        "nqhgd,nkhd->nhgqk", query_blocks, key_blocks, preferred_element_type=jnp.float32
    ) * head_width ** (-0.5)
    query_index = jnp.arange(window_len)[:, None]
    key_index = jnp.arange(2 * window_len)[None, :]
    offset_lag = window_len + query_index - key_index
    inband = (offset_lag >= 0) & (offset_lag < window_len)
    leading = (
        (jnp.arange(block_count)[:, None, None] > 0)
        | (key_index[None] >= window_len)
        | (lax.axis_index("sp") > 0)
    )
    valid = inband[None] & leading
    scores = jnp.where(valid[:, None, None], scores, -1e30)
    sink_rows = sink_logits.reshape(k_heads, group_size)[None, :, :, None]
    row_peak = jnp.maximum(jnp.max(scores, axis=-1), sink_rows)
    exp_terms = jnp.exp(scores - row_peak[..., None])
    denom_sum = jnp.sum(exp_terms, axis=-1) + jnp.exp(sink_rows - row_peak)
    weights = (exp_terms / denom_sum[..., None]).astype(jnp.bfloat16)
    attended = jnp.einsum(
        "nhgqk,nkhd->nqhgd", weights, value_blocks, preferred_element_type=jnp.float32
    ).astype(jnp.bfloat16)
    return attended.reshape(row_count, q_heads * head_width)


def per_device(
    queries,
    keys,
    values,
    query_gain,
    key_gain,
    sink_logits,
    out_weight,
    residual,
    norm_gain,
    gate_weight,
    up_weight,
    down_weight,
):
    n_sp, n_tp = lax.axis_size("sp"), lax.axis_size("tp")
    sp, tp = lax.axis_index("sp"), lax.axis_index("tp")
    half = (sp // PAIR) % 2
    row_count, width = residual.shape
    depth, units = gate_weight.shape
    units //= 2

    def part(array, axis, flip):
        return lax.dynamic_slice_in_dim(array, (half ^ flip) * units, units, axis)

    far = list(range(2 * PAIR, n_sp, 2))

    def send(first, second, flips):
        found = {}
        for flip in flips:
            other = (flip // PAIR) % 2
            if second is None:
                piece = part(first, 0, other)
            else:
                piece = jnp.concatenate([part(first, 1, other), part(second, 1, other)], axis=1)
            found[flip] = swap(piece, "sp", flip) if flip else piece
        return found

    def relay(found, flips):
        for flip in flips:
            found[flip ^ 1] = swap(found[flip], "sp", 1)

    edge = jnp.concatenate([keys, values], axis=1)[row_count - WINDOW :]
    edge = from_behind(edge, "sp", 1)
    gate_weight, up_weight, residual, out_weight, edge = lax.optimization_barrier(
        (gate_weight, up_weight, residual, out_weight, edge)
    )
    near = [0, PAIR]
    first = far[: len(far) // 2]
    residual_pair = swap(residual, "sp", PAIR)
    both = send(gate_weight, up_weight, first)
    both.update(send(gate_weight, up_weight, near))
    attended = attend(queries, keys, values, edge, query_gain, key_gain, sink_logits)
    attended_pair = swap(attended, "sp", PAIR)

    gate_weight, up_weight, down_weight, attended_pair = lax.optimization_barrier(
        (gate_weight, up_weight, down_weight, attended_pair)
    )
    both.update(send(gate_weight, up_weight, far[len(far) // 2 :]))
    early = {flip: both[flip] for flip in first}
    down_weight, early = lax.optimization_barrier((down_weight, early))
    both.update(early)
    down = send(down_weight, None, far)
    down.update(send(down_weight, None, near))
    relay(both, near + far)
    relay(down, near)

    gains = jnp.concatenate(gather_flips(norm_gain, "tp"))
    projections = gather_flips(out_weight, "tp")
    stream = jnp.concatenate([residual, residual_pair], axis=0)
    stream = jnp.concatenate(gather_flips(stream, "tp"), axis=1).astype(jnp.float32)
    heads = gather_flips(jnp.concatenate([attended, attended_pair], axis=0), "tp")

    def own_first(columns):
        pieces = [
            lax.dynamic_slice_in_dim(columns, (tp ^ flip) * width, width, 1)
            for flip in range(n_tp)
        ]
        return jnp.concatenate(pieces, axis=1)

    projection = jnp.concatenate([own_first(piece) for piece in projections], axis=0)
    head = jnp.concatenate(heads, axis=1)
    mixed = jnp.dot(head, projection, preferred_element_type=jnp.float32)
    middle = (stream + mixed).astype(jnp.bfloat16)
    middle = lax.optimization_barrier(middle)
    middle_wide = middle.astype(jnp.float32)
    mean = jnp.mean(middle_wide * middle_wide, axis=1, keepdims=True)
    normed = (middle_wide * lax.rsqrt(mean + 1e-06) * gains).astype(jnp.bfloat16)

    late = {flip: down[flip] for flip in far}
    normed, late = lax.optimization_barrier((normed, late))
    down.update(late)
    relay(down, far)

    per_part = width // depth

    def place(flip):
        block = sp ^ flip
        return (((block // per_part) ^ tp) * per_part + block % per_part) * depth

    flips = range(n_sp)
    normed_in = jnp.concatenate(
        [lax.dynamic_slice_in_dim(normed, place(flip), depth, 1) for flip in flips], axis=1
    )
    gate_full = jnp.concatenate([both[flip][:, :units] for flip in flips], axis=0)
    up_full = jnp.concatenate([both[flip][:, units:] for flip in flips], axis=0)
    gate_acts = jnp.dot(normed_in, gate_full, preferred_element_type=jnp.float32)
    up_acts = jnp.dot(normed_in, up_full, preferred_element_type=jnp.float32)
    hidden = (jax.nn.silu(gate_acts) * up_acts).astype(jnp.bfloat16)

    down_full = jnp.zeros((units, width * n_tp), jnp.bfloat16)
    for flip in flips:
        down_full = lax.dynamic_update_slice_in_dim(down_full, down[flip], place(flip), 1)
    terms = [
        jnp.dot(
            hidden, down_full[:, at * width : (at + 1) * width], preferred_element_type=jnp.float32
        ).astype(jnp.bfloat16)
        for at in range(n_tp)
    ]

    def add(one, other):
        return one.astype(jnp.float32) + other.astype(jnp.float32)

    flip = 1
    held = dict(enumerate(terms))
    while flip < n_tp // 2:
        held = {
            at: add(held[at], swap(held[at ^ flip], "tp", flip)).astype(jnp.bfloat16)
            for at in held
            if not at & flip
        }
        flip *= 2
    own, other = held[0], held[flip]
    cut = width // 2
    across = add(own[:, :cut], swap(other[:, :cut], "tp", flip)).astype(jnp.bfloat16)
    left = add(across[:row_count], swap(across[row_count:], "sp", PAIR))
    pair = jnp.concatenate([own[:, cut:], other[:, cut:]], axis=1)
    pair = add(pair[:row_count], swap(pair[row_count:], "sp", PAIR)).astype(jnp.bfloat16)
    right = add(pair[:, : width - cut], swap(pair[:, width - cut :], "tp", flip))
    feed = jnp.concatenate([left, right], axis=1)
    return (middle_wide[:row_count, :width] + 0.5 * feed).astype(jnp.bfloat16)


def solution(mesh):
    in_specs = (
        P("sp", "tp"),
        P("sp", "tp"),
        P("sp", "tp"),
        P(),
        P(),
        P("tp"),
        P("tp", None),
        P("sp", "tp"),
        P("tp"),
        P("sp", "tp"),
        P("sp", "tp"),
        P("tp", "sp"),
    )
    out_specs = P("sp", "tp")
    return jax.shard_map(
        per_device, mesh=mesh, in_specs=in_specs, out_specs=out_specs, check_vma=False
    )
```
